512 devices in a mesh: kv: 64 (over z, y), tp: 8 (over x, core).
Axes of the slice: x: 4, y: 8, z: 8, core: 2. Of those that a mesh axis runs over, the one named last changes fastest.
Arguments:
- hidden_in: bfloat16 [8, 1024], P(None, 'tp'), may hold values from -18 to 18, as said below
- input_gain: float32 [1024], P('tp'), may hold values from 0.1 to 1.9
- down_query: bfloat16 [1024, 256], P('tp'), may hold values from -0.1875 to 0.1875
- down_latent: bfloat16 [1024, 256], P('tp'), may hold values from -0.1875 to 0.1875
- down_rope: bfloat16 [1024, 64], P('tp'), may hold values from -0.1875 to 0.1875
- query_gain: float32 [256], replicated, may hold values from 0.1 to 1.9
- latent_gain: float32 [256], replicated, may hold values from 0.1 to 1.9
- up_query: bfloat16 [256, 8, 128], P(None, 'tp'), may hold values from -0.375 to 0.375
- up_rope: bfloat16 [256, 8, 64], P(None, 'tp'), may hold values from -0.375 to 0.375
- key_up: bfloat16 [256, 8, 128], P(None, 'tp'), may hold values from -0.375 to 0.375
- value_up: bfloat16 [256, 8, 128], P(None, 'tp'), may hold values from -0.375 to 0.375
- out_proj: bfloat16 [1024, 1024], P('tp', 'kv'), may hold values from -2 to 2, as said below
- output_gain: float32 [1024], P('kv'), may hold values from 0.1 to 1.9
- latent_cache: bfloat16 [8, 65536, 256], P(None, ('kv', 'tp')), may hold values from -6 to 6
- rope_cache: bfloat16 [8, 65536, 64], P(None, ('kv', 'tp')), may hold values from -6 to 6
- lengths: int32 [8], replicated, may hold values from 1 to 65536, as said below
Outputs:
- mixed: bfloat16 [8, 1024], P(None, 'kv')
The draws below stay inside these ranges and needn't reach their ends.
Inputs may be any that keep to these rules, and one draw needn't show every extreme that they name: Each length lies between 1 and 65536; in every draw some sequence has exactly 65536 and some exactly 1; lengths are heavily skewed toward short ones. `hidden_in`: activations whose size differs strongly between blocks of 64 features, by sequence. `out_proj`: output projection whose columns differ strongly in size.
All inputs are finite; a program needn't handle non-finite values.
Results may differ from the reference program's by a relative error of at most 0.015.
Values may be sent and summed in bfloat16 or wider, within the bound.
A program may use at most 128 MiB of HBM per device.

```python
import math
import jax
import jax.numpy as jnp
from jax import lax

D = 1024
H = 8
DN = 128
DR = 64
DV = 128
QR = 256
KR = 256
SEQS = 8
LEN = 65536


def draw_lengths(key, part):
    subkeys = jax.random.split(key, 3)
    drawn = jax.random.randint(subkeys[0], (SEQS,), 1, LEN + 1)
    shifts = jax.random.randint(subkeys[1], (SEQS,), 0, LEN.bit_length())
    result = jnp.maximum(jnp.right_shift(drawn, shifts), 1)
    chosen = jax.random.randint(subkeys[2], (), 0, SEQS)
    result = result.at[chosen].set(LEN)
    result = result.at[(chosen + 1) % SEQS].set(1)
    return result.astype(jnp.int32)


def draw_hidden_in(key, part):
    subkeys = jax.random.split(jax.random.fold_in(key, 11), 2)
    blocks = D // 64
    base = jnp.clip(jax.random.normal(subkeys[0], (SEQS, blocks, 64), jnp.float32), -4.0, 4.0)
    spread = jnp.exp(jax.random.uniform(subkeys[1], (SEQS, blocks, 1), jnp.float32, -1.5, 1.5))
    return (base * spread).reshape(SEQS, D).astype(jnp.bfloat16)


def draw_out_proj(key, part):
    subkeys = jax.random.split(jax.random.fold_in(key, 23), 2)
    base = jnp.clip(jax.random.normal(subkeys[0], (H * DV, D), jnp.float32), -4.0, 4.0)
    spread = jnp.exp(jax.random.uniform(subkeys[1], (1, D), jnp.float32, -1.5, 1.5))
    return (base * spread / jnp.sqrt(jnp.float32(H * DV))).astype(jnp.bfloat16)


def shard_levels(own_key, extent, cuts, least, high):
    level, own = 1.0, jax.random.fold_in(own_key, 6)
    for dim, parts in cuts:
        steps = jnp.exp(jax.random.uniform(jax.random.fold_in(own, dim), (parts,), jnp.float32, least / len(cuts), high / len(cuts)))
        level = level * jnp.repeat(steps, extent[dim] // parts).reshape([-1 if axis == dim else 1 for axis in range(len(extent))])
    return level


def centred(rng, dims, width, bound, pieces=(), kind=jnp.bfloat16):
    loudness = shard_levels(rng, dims, pieces, -0.22, 0.18) if pieces else 1.0
    values = jax.random.normal(rng, dims, jnp.float32) * width * loudness
    return jnp.minimum(jnp.maximum(values, -bound), bound).astype(kind)


def setup_inputs(seed: int = 0) -> dict:
    seeds = jax.random.split(jax.random.key(seed), 17)
    return {
        "hidden_in": draw_hidden_in(jax.random.fold_in(seeds[16], 71), 0),
        "input_gain": jnp.clip(1.0 + 0.18 * jax.random.normal(seeds[1], (D,), jnp.float32), 0.1, 1.9),
        "down_query": centred(seeds[2], (D, QR), D ** -0.5, 0.1875, ((0, 8),)),
        "down_latent": centred(seeds[3], (D, KR), D ** -0.5, 0.1875, ((0, 8),)),
        "down_rope": centred(seeds[4], (D, DR), D ** -0.5, 0.1875, ((0, 8),)),
        "query_gain": jnp.clip(1.0 + 0.18 * jax.random.normal(seeds[5], (QR,), jnp.float32), 0.1, 1.9),
        "latent_gain": jnp.clip(1.0 + 0.18 * jax.random.normal(seeds[6], (KR,), jnp.float32), 0.1, 1.9),
        "up_query": centred(seeds[7], (QR, H, DN), QR ** -0.5, 0.375, ((1, 8),)),
        "up_rope": centred(seeds[8], (QR, H, DR), QR ** -0.5, 0.375, ((1, 8),)),
        "key_up": centred(seeds[9], (KR, H, DN), KR ** -0.5, 0.375, ((1, 8),)),
        "value_up": centred(seeds[10], (KR, H, DV), KR ** -0.5, 0.375, ((1, 8),)),
        "out_proj": draw_out_proj(jax.random.fold_in(seeds[16], 71), 0),
        "output_gain": jnp.clip(1.0 + 0.18 * jax.random.normal(seeds[12], (D,), jnp.float32), 0.1, 1.9),
        "latent_cache": centred(seeds[13], (SEQS, LEN, KR), 1.0, 6.0, ((1, 512),)),
        "rope_cache": centred(seeds[14], (SEQS, LEN, DR), 1.0, 6.0, ((1, 512),)),
        "lengths": draw_lengths(jax.random.fold_in(seeds[16], 71), 0),
    }


THETA = 10000.0
EPSILON = 1e-06

def rotate(values, angles):
    half_width = values.shape[-1] // 2
    first_half = values[..., :half_width]
    second_half = values[..., half_width:]
    cosine = jnp.cos(angles)
    sine_part = jnp.sin(angles)
    return jnp.concatenate([first_half * cosine - second_half * sine_part, second_half * cosine + first_half * sine_part], axis=-1)

def angles_for(positions, rot_width):
    inverse = 1.0 / THETA ** (jnp.arange(0, rot_width, 2, dtype=jnp.float32) / rot_width)
    return positions[:, None] * inverse[None, :]

def normed(values, gain_row):
    return values * lax.rsqrt(lax.optimization_barrier(jnp.mean(values * values, axis=-1, keepdims=True)) + EPSILON) * gain_row.astype(jnp.float32)

def widen(values):
    return values.astype(jnp.float32)

def settle(values):
    return lax.optimization_barrier(values.astype(jnp.bfloat16))

def reference(hidden_in, input_gain, down_query, down_latent, down_rope, query_gain, latent_gain, up_query, up_rope, key_up, value_up, out_proj, output_gain, latent_cache, rope_cache, lengths):
    floats = widen(hidden_in)
    inv_rms = lax.rsqrt(lax.optimization_barrier(jnp.mean(floats * floats, axis=1, keepdims=True)) + EPSILON)
    scaled = (floats * widen(input_gain)).astype(jnp.bfloat16)
    query_low = jnp.dot(scaled, down_query, preferred_element_type=jnp.float32) * inv_rms
    latent_low = jnp.dot(scaled, down_latent, preferred_element_type=jnp.float32) * inv_rms
    rope_low = jnp.dot(scaled, down_rope, preferred_element_type=jnp.float32) * inv_rms
    positions = lengths.astype(jnp.float32)
    query_normed = settle(normed(query_low, query_gain))
    query_nope = settle(jnp.einsum('bq,qhd->bhd', widen(query_normed), widen(up_query)))
    query_rope = jnp.einsum('bq,qhr->bhr', widen(query_normed), widen(up_rope))
    query_rope = settle(rotate(query_rope, angles_for(positions, DR)[:, None, :]))
    latent_query = settle(jnp.einsum('bhd,chd->bhc', widen(query_nope), widen(key_up)))
    latent_new = settle(normed(latent_low, latent_gain))
    rope_new = settle(rotate(rope_low, angles_for(positions, DR)))
    factor = 1.0 / math.sqrt(DN + DR)
    places = jnp.arange(LEN, dtype=jnp.int32)

    def one_sequence(inputs):
        seq_query, seq_rope, latents, rotated, fresh_latent, fresh_rope, length = inputs
        scores = (jnp.einsum('hc,pc->hp', widen(seq_query), widen(latents)) + jnp.einsum('hr,pr->hp', widen(seq_rope), widen(rotated))) * factor
        usable = places < length
        scores = jnp.where(usable[None, :], scores, -1e+30)
        new_score = (lax.optimization_barrier(jnp.sum(widen(seq_query) * widen(fresh_latent)[None, :], axis=-1)) + lax.optimization_barrier(jnp.sum(widen(seq_rope) * widen(fresh_rope)[None, :], axis=-1))) * factor
        highest = jnp.maximum(lax.optimization_barrier(jnp.max(scores, axis=-1)), new_score)
        weights = jnp.where(usable[None, :], jnp.exp(scores - highest[:, None]), 0.0)
        fresh_weight = jnp.exp(new_score - highest)
        total_mass = lax.optimization_barrier(jnp.sum(weights, axis=-1)) + fresh_weight
        summed = jnp.einsum('hp,pc->hc', widen(settle(weights)), widen(latents)) + fresh_weight[:, None] * widen(fresh_latent)[None, :]
        return summed / total_mass[:, None]
    attended = lax.map(one_sequence, (latent_query, query_rope, latent_cache, rope_cache, latent_new, rope_new, lengths))
    attended = settle(attended)
    values_out = settle(jnp.einsum('bhc,chv->bhv', widen(attended), widen(value_up)))
    flattened = values_out.reshape(values_out.shape[0], H * DV)
    out_full = jnp.dot(flattened, out_proj, preferred_element_type=jnp.float32)
    out_rms = lax.rsqrt(lax.optimization_barrier(jnp.mean(out_full * out_full, axis=1, keepdims=True)) + EPSILON)
    return (out_full * out_rms * widen(output_gain)).astype(jnp.bfloat16)
```

```python
import functools
import math

import jax
import jax.numpy as jnp
import numpy as np
from jax import lax
from jax.experimental import pallas as pl
from jax.experimental.pallas import tpu as pltpu
from jax.sharding import PartitionSpec as P

THETA = 10000.0
EPSILON = 1e-06
MESH = pl.DeviceIdType.MESH
F32 = jnp.float32
BF16 = jnp.bfloat16
NT = (((1,), (1,)), ((), ()))
Y = 8
RING = (4, 3, 5, 2, 6, 1, 7)


def iota(shape, dim):
    return lax.broadcasted_iota(jnp.int32, shape, dim)


def dot(a, b):
    return jnp.dot(a, b, preferred_element_type=F32)


def dot_nt(a, b):
    return lax.dot_general(a, b, NT, preferred_element_type=F32)


def sin_cos(x):
    turns = jnp.floor(x * (1.0 / (2 * math.pi)) + 0.5)
    r = (x - turns * 6.28125) - turns * (2 * math.pi - 6.28125)
    r2 = r * r
    s = jnp.full_like(x, 1.0)
    for n in (15, 13, 11, 9, 7, 5, 3):
        s = 1.0 - s * r2 * (1.0 / (n * (n - 1)))
    c = jnp.full_like(x, 1.0)
    for n in (18, 16, 14, 12, 10, 8, 6, 4, 2):
        c = 1.0 - c * r2 * (1.0 / (n * (n - 1)))
    return s * r, c


def kernel(
    K,
    T,
    lengths_h,
    inverse_h,
    hidden_h,
    gain_h,
    dq_h,
    dl_h,
    dr_h,
    qg_h,
    lg_h,
    uq_h,
    ur_h,
    ku_h,
    vu_h,
    op_h,
    lat_h,
    rope_h,
    out,
    hidden,
    gain,
    dq,
    dl,
    dr,
    qg,
    lg,
    uq,
    ur,
    ku,
    vu,
    lat,
    rope,
    op,
    absorbed,
    rx1,
    rx2,
    tx3,
    rx3,
    rxy,
    rxz,
    rx6,
    lengths,
    inverse,
    load_sem,
    send_sem,
    recv_sem,
):
    Z = K // Y
    B, D = hidden.shape[0], hidden.shape[1] * T
    QR, KR, DR = dq.shape[1], dl.shape[1], dr.shape[0]
    DN, DV = uq.shape[1], vu.shape[1]
    span = lat.shape[1]
    cols = op.shape[2]
    k = lax.axis_index("kv")
    t = lax.axis_index("tp")
    z, y = k // Y, lax.rem(k, Y)
    factor = 1.0 / math.sqrt(DN + DR)

    def peer(axis, i):
        if axis == "x":
            return (k, lax.rem(t + i, T))
        if axis == "y":
            return (z * Y + lax.rem(y + i, Y), t)
        return (lax.rem(z + i, Z) * Y + y, t)

    barrier = pltpu.get_barrier_semaphore()
    for i in RING:
        for axis in "yzx":
            pl.semaphore_signal(barrier, inc=1, device_id=peer(axis, i), device_id_type=MESH)

    pairs = (
        (hidden_h, hidden), (gain_h, gain), (dq_h, dq), (dl_h, dl), (dr_h, dr),
        (op_h, op.at[z, y]), (lengths_h, lengths), (inverse_h, inverse),
        (uq_h, uq), (ku_h, ku), (ur_h, ur.at[pl.ds(0, DR)]), (qg_h, qg), (lg_h, lg), (vu_h, vu),
        (lat_h, lat), (rope_h, rope.at[:, pl.ds(0, DR)]), (rope_h, rope.at[:, pl.ds(DR, DR)]),
    )
    loads = [pltpu.make_async_copy(a, b, load_sem.at[i]) for i, (a, b) in enumerate(pairs)]
    for load in loads:
        load.start()

    def send(phase, axis, src, dst):
        for i in RING:
            pltpu.make_async_remote_copy(
                src_ref=src(i),
                dst_ref=dst,
                send_sem=send_sem.at[phase],
                recv_sem=recv_sem.at[phase],
                device_id=peer(axis, i),
                device_id_type=MESH,
            ).start()

    def drain(buffer, sem):
        pltpu.make_async_copy(buffer.at[pl.ds(0, 7)], buffer.at[pl.ds(0, 7)], sem).wait()

    for load in loads[:5]:
        load.wait()
    floats = hidden[...].astype(F32)
    scaled = (floats * gain[...]).astype(BF16)
    squares = jnp.sum(floats * floats, axis=1, keepdims=True)
    low = rx1.at[t]
    low[...] = jnp.concatenate(
        [
            dot(scaled, dq[...]),
            dot(scaled, dl[...]),
            dot_nt(scaled, dr[...]),
            jnp.broadcast_to(squares, (B, rx1.shape[2] - QR - KR - DR)),
        ],
        axis=1,
    ).astype(BF16)
    loads[5].wait()
    pl.semaphore_wait(barrier, 21)
    send(0, "x", lambda i: rx1.at[t], rx1.at[t])
    send(6, "y", lambda i: op.at[z, y], op.at[z, y])

    for load in loads[6:]:
        load.wait()
    absorbed[...] = dot_nt(uq[...], ku[...]).astype(BF16)
    half = DR // 2
    turned = ur[:DR].astype(F32)
    ur[DR:] = jnp.concatenate([-turned[half:], turned[:half]], axis=0).astype(BF16)
    seq = iota((B, DR), 0)
    position = jnp.zeros((B, DR), F32)
    for b in range(B):
        position = jnp.where(seq == b, lengths[b].astype(F32), position)
    sine, cosine = sin_cos(position * inverse[...])
    rotary = jnp.concatenate([cosine, sine], axis=1)
    rows = lax.rem(iota((T * B, span), 0), B)
    limit = jnp.zeros((T * B, span), jnp.int32)
    for b in range(B):
        limit = jnp.where(rows == b, lengths[b], limit)
    usable = iota((T * B, span), 1) + (k * T + t) * span < limit

    drain(rx1, recv_sem.at[0])
    total = rx1[0].astype(F32)
    for i in range(1, T):
        total = total + rx1[i].astype(F32)
    inv2 = 1.0 / (total[:, QR + KR + DR : QR + KR + DR + 1] / D + EPSILON)
    inv = jnp.sqrt(inv2)

    def low_norm(v, g):
        mean = jnp.mean(v * v, axis=-1, keepdims=True) * inv2
        return v * (inv * lax.rsqrt(mean + EPSILON)) * g

    query_normed = low_norm(total[:, :QR], qg[...]).astype(BF16)
    own_latent = dot(query_normed, absorbed[...])
    own_rope = dot_nt(query_normed, ur[...]) * rotary
    query = jnp.concatenate([own_latent, own_rope], axis=1)
    rx2[t] = query.astype(BF16)
    send(1, "x", lambda i: rx2.at[t], rx2.at[t])

    drain(op.at[z], recv_sem.at[6])
    send(7, "z", lambda i: op.at[z], op.at[z])
    latent_new = low_norm(total[:, QR : QR + KR], lg[...]).astype(BF16)
    rope_low = total[:, QR + KR : QR + KR + DR] * inv
    swapped = jnp.concatenate([-rope_low[:, half:], rope_low[:, :half]], axis=1)
    rope_new = (rope_low * cosine + swapped * sine).astype(BF16).astype(F32)
    rope_new = jnp.concatenate([rope_new, rope_new], axis=1)
    rounded = query.astype(BF16).astype(F32)
    new_score = (
        jnp.sum(rounded[:, :KR] * latent_new.astype(F32), axis=1, keepdims=True)
        + jnp.sum(rounded[:, KR:] * rope_new, axis=1, keepdims=True)
    ) * factor
    new_value = dot(latent_new, vu[...])

    drain(rx2, recv_sem.at[1])
    queries = rx2[...].astype(F32).reshape(T * B, rx2.shape[2]).astype(BF16)
    scores = jnp.zeros((T * B, span), F32)
    for b in range(B):
        part = dot_nt(queries[:, :KR], lat[b]) + dot(queries[:, KR:], rope[b])
        scores = jnp.where(rows == b, part, scores)
    scores = jnp.where(usable, scores * factor, -1e30)
    top = jnp.max(scores, axis=1, keepdims=True).astype(BF16).astype(F32)
    weights = jnp.where(usable, jnp.exp(scores - top), 0.0)
    mass = jnp.sum(weights, axis=1, keepdims=True)
    summed = jnp.zeros((T * B, KR), F32)
    for b in range(B):
        summed = summed + dot(jnp.where(rows == b, weights, 0.0).astype(BF16), lat[b])
    mark = iota((T * B, 128), 1)
    tail = jnp.where(mark == 0, top, mass)
    block = jnp.concatenate([summed, tail], axis=1)
    tx3[...] = block.reshape(T, B, KR + 128).astype(BF16)
    send(2, "x", lambda i: tx3.at[lax.rem(t + i, T)], rx3.at[t])
    rx3[t] = tx3[t]
    drain(rx3, recv_sem.at[2])

    mark = iota((B, 128), 1)

    def combine(buffer, n):
        parts = buffer[...].astype(F32)
        tops = parts[:, :, n : n + 1]
        highest = jnp.max(tops, axis=0)
        scale = jnp.exp(tops - highest)
        return jnp.sum(parts * scale, axis=0), highest

    def share(phase, axis, buffer, slot, value, mass, highest):
        tail = jnp.where(mark == 0, highest, mass)
        buffer[slot] = jnp.concatenate([value, tail], axis=1).astype(BF16)
        send(phase, axis, lambda i: buffer.at[slot], buffer.at[slot])
        drain(buffer, recv_sem.at[phase])

    total, highest = combine(rx3, KR)
    value = dot(total[:, :KR].astype(BF16), vu[...])
    share(3, "y", rxy, y, value, total[:, KR:], highest)
    total, highest = combine(rxy, DV)
    share(4, "z", rxz, z, total[:, :DV], total[:, DV:], highest)
    total, highest = combine(rxz, DV)
    final = jnp.maximum(highest, new_score)
    old = jnp.exp(highest - final)
    fresh = jnp.exp(new_score - final)
    mass = total[:, DV + 1 : DV + 2] * old + fresh
    value = ((total[:, :DV] * old + new_value * fresh) / mass).astype(BF16)

    drain(op, recv_sem.at[7])
    everything = op[...].reshape(K * cols, DV)
    own = jnp.concatenate([op[z, y], jnp.zeros((128 - cols, DV), BF16)], axis=0)
    rx6[t] = jnp.concatenate([dot_nt(value, everything), dot_nt(value, own)], axis=1).astype(BF16)
    send(5, "x", lambda i: rx6.at[t], rx6.at[t])
    drain(rx6, recv_sem.at[5])
    total = rx6[0].astype(F32)
    for i in range(1, T):
        total = total + rx6[i].astype(F32)
    full = total[:, : K * cols]
    mean = jnp.mean(full * full, axis=1, keepdims=True)
    out[...] = total[:, K * cols : K * cols + cols] * lax.rsqrt(mean + EPSILON)

    for phase, buffer in enumerate((rx1, rx2, rx3, rxy, rxz, rx6, op.at[z], op)):
        drain(buffer, send_sem.at[phase])


def shards(
    K, T, hidden_in, input_gain, down_query, down_latent, down_rope, query_gain, latent_gain,
    up_query, up_rope, key_up, value_up, out_proj, output_gain, latent_cache, rope_cache, lengths,
):
    B = hidden_in.shape[0]
    QR, Hd, DN = up_query.shape
    KR, DR, DV = key_up.shape[0], up_rope.shape[2], value_up.shape[2]
    span, cols = latent_cache.shape[1], out_proj.shape[1]
    steps = np.arange(0, DR, 2, dtype=np.float64) / DR
    inverse = np.tile((1.0 / THETA**steps).astype(np.float32), 2)[None, :]
    flat = lambda w: w.reshape(w.shape[0] * w.shape[1], w.shape[2])
    row = lambda v: v.reshape(1, v.shape[0])
    arrays = (
        hidden_in, row(input_gain), down_query, down_latent, down_rope.T, row(query_gain),
        row(latent_gain), flat(up_query), flat(up_rope.transpose(1, 2, 0)), flat(key_up),
        flat(value_up), out_proj.T, latent_cache, rope_cache.transpose(0, 2, 1),
    )
    vm = lambda *shape: pltpu.VMEM(shape, BF16)
    low = -(-(QR + KR + DR + 1) // 128) * 128
    dma = pltpu.SemaphoreType.DMA
    scratch = [
        vm(*hidden_in.shape),
        pltpu.VMEM((1, input_gain.shape[0]), F32),
        vm(*down_query.shape),
        vm(*down_latent.shape),
        vm(DR, down_rope.shape[0]),
        pltpu.VMEM((1, QR), F32),
        pltpu.VMEM((1, KR), F32),
        vm(QR, DN),
        vm(2 * DR, QR),
        vm(KR, DN),
        vm(KR, DV),
        vm(B, span, KR),
        vm(B, 2 * DR, span),
        vm(K // Y, Y, cols, DV),
        vm(QR, KR),
        vm(T, B, low),
        vm(T, B, KR + 128),
        vm(T, B, KR + 128),
        vm(T, B, KR + 128),
        vm(Y, B, DV + 128),
        vm(K // Y, B, DV + 128),
        vm(T, B, K * cols + 128),
        pltpu.SMEM(lengths.shape, lengths.dtype),
        pltpu.VMEM(inverse.shape, F32),
        dma((len(arrays) + 3,)),
        dma((8,)),
        dma((8,)),
    ]
    normal = pl.pallas_call(
        functools.partial(kernel, K, T),
        out_shape=jax.ShapeDtypeStruct((B, cols), F32),
        in_specs=[pl.BlockSpec(memory_space=pl.ANY)] * (len(arrays) + 2),
        out_specs=pl.BlockSpec(memory_space=pltpu.VMEM),
        scratch_shapes=scratch,
        compiler_params=pltpu.CompilerParams(collective_id=0, has_side_effects=True),
    )(lengths, jnp.asarray(inverse), *arrays)
    return (normal * row(output_gain)).astype(BF16)


def solution(mesh):
    in_specs = (
        P(None, "tp"),
        P("tp"),
        P("tp", None),
        P("tp", None),
        P("tp", None),
        P(),
        P(),
        P(None, "tp", None),
        P(None, "tp", None),
        P(None, "tp", None),
        P(None, "tp", None),
        P("tp", "kv"),
        P("kv"),
        P(None, ("kv", "tp"), None),
        P(None, ("kv", "tp"), None),
        P(),
    )
    body = functools.partial(shards, mesh.shape["kv"], mesh.shape["tp"])
    return jax.shard_map(body, mesh=mesh, in_specs=in_specs, out_specs=P(None, "kv"), check_vma=False)
```
